32 devices in a mesh: sp: 16 (over z, y, x), tp: 2 (over core).
Axes of the slice: x: 2, y: 2, z: 4, core: 2. Of those that a mesh axis runs over, the one named last changes fastest.
Arguments:
- residual: bfloat16 [4096, 2048], P(('sp', 'tp')), may hold values from -6 to 6
- projected: bfloat16 [4096, 2048], P('sp', 'tp'), may hold values from -6 to 6
- group_weight: bfloat16 [4, 512, 512], P('tp'), may hold values from -0.25 to 0.25
- channel_scale: float32 [2048], P('tp'), may hold values from 0.1 to 1.9
- out_weight: bfloat16 [2048, 2048], replicated, may hold values from -0.125 to 0.125
- post_mix_gain: float32 [2048], replicated, may hold values from 0.1 to 1.9
- pre_ffn_gain: float32 [2048], replicated, may hold values from 0.1 to 1.9
- post_ffn_gain: float32 [2048], replicated, may hold values from 0.1 to 1.9
- route_ids: int32 [4096, 2], P(('sp', 'tp')), may hold values from 0 to 7, all different within a row; in each aligned block of 128 rows (0 to 127, 128 to 255, ...) at most 64 rows name the same one
- route_weight: float32 [4096, 2], P(('sp', 'tp')), may hold values from 0.1 to 1
- expert_gate: bfloat16 [16, 2048, 1792], P('sp', None, 'tp'), may hold values from -0.125 to 0.125
- expert_up: bfloat16 [16, 2048, 1792], P('sp', None, 'tp'), may hold values from -0.125 to 0.125
- expert_down: bfloat16 [16, 1792, 2048], P('sp', 'tp'), may hold values from -0.09375 to 0.09375
Outputs:
- layer_out: bfloat16 [4096, 2048], P(('sp', 'tp'))
The draws below stay inside these ranges and needn't reach their ends.
Inputs may be any that keep to these rules, and one draw needn't show every extreme that they name: `route_ids`: each row names 2 different experts. In every aligned block of 128 rows (the rows of one device) no expert is named more than 64 times, a bound that some blocks reach.
All inputs are finite; a program needn't handle non-finite values.
Results may differ from the reference program's by a relative error of at most 0.014.
Values may be sent and summed in bfloat16 or wider, within the bound.
No kernel may reach another device: no remote copies, remote signals or barrier semaphores. Data moves between devices by JAX's collectives and lax.ppermute only.
A program may use at most 192 MiB of HBM per device.

```python
import math
import jax
import jax.numpy as jnp
import numpy as np
from jax import lax

D = 2048
GROUPS = 4
GROUP_W = 512
FF = 3584
TOP = 2
TOKENS = 4096
ROWS_DEV = 128
EXPERTS = 8
HALVES = 16
CAP = 64
N_SP = 16
N_TP = 2


def steps_of(key, extent, split, low, top_value):
    loudness, own = 1.0, jax.random.fold_in(key, 6)
    for dim, parts in split:
        heights = jnp.exp(jax.random.uniform(jax.random.fold_in(own, dim), (parts,), jnp.float32, low / len(split), top_value / len(split)))
        loudness = loudness * jnp.repeat(heights, extent[dim] // parts).reshape([-1 if axis == dim else 1 for axis in range(len(extent))])
    return loudness


def assign_block(key, own, number, rows, number_of, top, limit, slope):
    sequence = jax.random.permutation(key, number_of)
    heavy_load, usual = load_shares(number_of, rows * top, limit, slope, True), load_shares(number_of, rows * top, limit, slope, False)
    places = jnp.arange(number_of)

    def named(sizes, rotation):
        used = int((sizes > 0).sum())
        fixed = max(1, used // 4)
        passed = fixed + (places - fixed + rotation * (used - fixed)) % max(1, number_of - fixed)
        return jnp.zeros((number_of,), jnp.int32).at[sequence[jnp.where(places < fixed, places, passed)]].set(jnp.asarray(sizes, jnp.int32))

    sizes = jnp.where(number % 4 == 0, named(heavy_load, number // 4), named(usual, number - number // 4 - 1))
    mixed = jax.random.permutation(jax.random.fold_in(own, 3), number_of)
    giver, receiver = mixed[0:number_of // 2 * 2:2], mixed[1:number_of // 2 * 2:2]
    margin = jnp.minimum(sizes[giver] - 1, limit - sizes[receiver]) // 2
    margin = jnp.where((giver == sequence[0]) | (receiver == sequence[0]) | (sizes[receiver] == 0), 0, jnp.maximum(margin, 0))
    passed = jax.random.randint(jax.random.fold_in(own, 4), (number_of // 2,), 0, 1 << 20) % (margin + 1)
    sizes = sizes.at[giver].add(-passed).at[receiver].add(passed)
    members = jnp.searchsorted(jnp.cumsum(sizes), jnp.arange(rows * top), side="right").astype(jnp.int32)
    listing = members.reshape(top, rows).T
    listing = listing[jax.random.permutation(jax.random.fold_in(own, 1), rows)]
    rotation = jax.random.randint(jax.random.fold_in(own, 2), (rows, 1), 0, top)
    return jnp.take_along_axis(listing, (jnp.arange(top)[None, :] + rotation) % top, axis=1)


def load_shares(number_of, total, most, slope, full):
    weights = [(1 << 20) // math.isqrt(grade ** slope) + 1 for grade in range(1, number_of + 1)]
    largest = most if full else min(most, max(-(-total // number_of), total * weights[0] // sum(weights)))
    least = 1 if total - largest >= number_of - 1 else 0
    given, spare = [largest] + [least] * (number_of - 1), total - largest - least * (number_of - 1)
    while spare > 0:
        movable = [i for i in range(1, number_of) if given[i] < largest] or [i for i in range(1, number_of) if given[i] < most]
        pool, remaining = sum([weights[i] for i in movable]), spare
        for i in movable:
            extra = min(most - given[i], max(1, remaining * weights[i] // pool), spare)
            given[i] = given[i] + extra
            spare = spare - extra
    return np.array(given)


def scatter_about(rng, dims, width, limit, shards=(), kind=jnp.bfloat16):
    result = jax.random.normal(rng, dims, jnp.float32) * width
    if len(shards) > 0:
        result = steps_of(rng, dims, shards, -0.22, 0.18) * result
    return jnp.clip(result, min=-limit, max=limit).astype(kind)


def setup_inputs(seed: int = 0) -> dict:
    keys = jax.random.split(jax.random.key(seed), 14)
    residual = scatter_about(keys[0], (TOKENS, D), 1.0, 6.0, ((0, 32),))
    projected = scatter_about(keys[1], (TOKENS, D), 1.0, 6.0, ((0, 16), (1, 2)))
    group_weight = scatter_about(keys[2], (GROUPS, GROUP_W, GROUP_W), GROUP_W ** -0.5, 0.25, ((0, 2),))
    channel_scale = jnp.clip(1.0 + 0.18 * jax.random.normal(keys[3], (D,), jnp.float32), 0.1, 1.9)
    out_weight = scatter_about(keys[4], (D, D), D ** -0.5, 0.125)
    post_mix_gain = jnp.clip(1.0 + 0.18 * jax.random.normal(keys[5], (D,), jnp.float32), 0.1, 1.9)
    pre_ffn_gain = jnp.clip(1.0 + 0.18 * jax.random.normal(keys[6], (D,), jnp.float32), 0.1, 1.9)
    post_ffn_gain = jnp.clip(1.0 + 0.18 * jax.random.normal(keys[7], (D,), jnp.float32), 0.1, 1.9)
    route_ids_keys = jax.random.split(jax.random.fold_in(keys[8], 1), TOKENS // ROWS_DEV)
    route_ids_turns = jax.random.permutation(jax.random.fold_in(keys[8], 3), TOKENS // ROWS_DEV)
    route_ids = jax.vmap(lambda own, number: assign_block(jax.random.fold_in(keys[8], 2), own, number, ROWS_DEV, EXPERTS, TOP, CAP, 2))(route_ids_keys, route_ids_turns).reshape((TOKENS, TOP))
    route_weight = jnp.clip(0.1 + 0.9 * jax.random.uniform(keys[9], (TOKENS, TOP), jnp.float32) ** steps_of(keys[9], (TOKENS, TOP), ((0, 32),), -0.2, 0.2), 0.1, 1.0)
    expert_gate = scatter_about(keys[10], (HALVES, D, FF // 2), D ** -0.5, 0.125, ((0, 16), (2, 2)))
    expert_up = scatter_about(keys[11], (HALVES, D, FF // 2), D ** -0.5, 0.125, ((0, 16), (2, 2)))
    expert_down = scatter_about(keys[12], (HALVES, FF // 2, D), FF ** -0.5, 0.09375, ((0, 16), (1, 2)))
    return dict(residual=residual, projected=projected, group_weight=group_weight, channel_scale=channel_scale, out_weight=out_weight, post_mix_gain=post_mix_gain, pre_ffn_gain=pre_ffn_gain, post_ffn_gain=post_ffn_gain, route_ids=route_ids, route_weight=route_weight, expert_gate=expert_gate, expert_up=expert_up, expert_down=expert_down)


EPS = 1e-06

def rms_scale(values, gain):
    values = values.astype(jnp.float32)
    inverse = lax.rsqrt(lax.optimization_barrier(jnp.mean(values * values, axis=-1, keepdims=True)) + EPS)
    return values * inverse * gain.astype(jnp.float32)

def window_sums(extended, lookback, count):
    levels = []
    current = extended
    window_span = 1
    for level_id in range(GROUPS):
        current = current[window_span:] + current[:-window_span]
        window_span = window_span * 2
        first = lookback - window_span + 1
        levels.append(lax.slice_in_dim(current, first, first + count, axis=0))
    return levels

def expert_output(token_rows, expert_id, expert_gate, expert_up, expert_down):
    quarter = FF // (2 * N_TP)
    total = jnp.zeros((token_rows.shape[0], D), jnp.float32)
    for half_id in range(2):
        entry = (2 * expert_id + half_id).astype(jnp.int32)
        gate_half = lax.dynamic_index_in_dim(expert_gate, entry, 0, keepdims=False)
        up_half = lax.dynamic_index_in_dim(expert_up, entry, 0, keepdims=False)
        down_half = lax.dynamic_index_in_dim(expert_down, entry, 0, keepdims=False)
        partial_value = jnp.zeros((token_rows.shape[0], D), jnp.float32)
        for part_id in range(N_TP):
            low = part_id * quarter
            gate_value = jnp.dot(token_rows, gate_half[:, low:low + quarter], preferred_element_type=jnp.float32)
            up_value = jnp.dot(token_rows, up_half[:, low:low + quarter], preferred_element_type=jnp.float32)
            active = (jax.nn.silu(gate_value) * up_value).astype(jnp.bfloat16)
            term = jnp.dot(active, down_half[low:low + quarter], preferred_element_type=jnp.float32).astype(jnp.bfloat16)
            partial_value = partial_value + term.astype(jnp.float32)
        total = total + partial_value.astype(jnp.bfloat16).astype(jnp.float32)
    rounded = lax.optimization_barrier(total.astype(jnp.bfloat16))
    return rounded.astype(jnp.float32)

def reference(residual, projected, group_weight, channel_scale, out_weight, post_mix_gain, pre_ffn_gain, post_ffn_gain, route_ids, route_weight, expert_gate, expert_up, expert_down):
    lookback = 2 ** GROUPS
    count = projected.shape[0]
    extended = jnp.concatenate([jnp.zeros((lookback, D), jnp.float32), projected.astype(jnp.float32)], 0)
    levels = window_sums(extended, lookback, count)
    position = (jnp.arange(count, dtype=jnp.int32) + 1).astype(jnp.float32)[:, None]
    pieces = []
    for group_id in range(GROUPS):
        low = group_id * GROUP_W
        window_span = jnp.float32(2.0 ** (group_id + 1))
        own_part = projected[:, low:low + GROUP_W].astype(jnp.float32)
        pieces.append(levels[group_id][:, low:low + GROUP_W] / jnp.minimum(position, window_span) - own_part)
    pooled = jnp.concatenate(pieces, 1).astype(jnp.bfloat16)
    grouped = jnp.einsum('tgc,gce->tge', pooled.reshape(count, GROUPS, GROUP_W).astype(jnp.float32), group_weight.astype(jnp.float32))
    scaled = (grouped.reshape(count, D) * channel_scale.astype(jnp.float32)).astype(jnp.bfloat16)
    mixed = jnp.dot(scaled, out_weight, preferred_element_type=jnp.float32).astype(jnp.bfloat16)
    middle = (residual.astype(jnp.float32) + rms_scale(mixed, post_mix_gain)).astype(jnp.bfloat16)
    normed = rms_scale(middle, pre_ffn_gain).astype(jnp.bfloat16)
    flat_ids = route_ids.reshape(-1).astype(jnp.int32)
    flat_weight = route_weight.reshape(-1).astype(jnp.float32)
    order = jnp.argsort(flat_ids, stable=True).astype(jnp.int32)
    onehot = (flat_ids[:, None] == jnp.arange(EXPERTS, dtype=jnp.int32)[None, :]).astype(jnp.int32)
    counts = lax.optimization_barrier(jnp.sum(onehot, 0)).astype(jnp.int32)
    starts = (jnp.cumsum(counts) - counts).astype(jnp.int32)
    most = CAP * N_SP * N_TP
    order_padded = jnp.concatenate([order, jnp.zeros((most,), jnp.int32)])

    def add_expert(total, expert_id):
        picks = lax.dynamic_slice_in_dim(order_padded, starts[expert_id].astype(jnp.int32), most)
        live = jnp.arange(most, dtype=jnp.int32) < counts[expert_id]
        token_ids = (picks // TOP).astype(jnp.int32)
        outputs = expert_output(normed[token_ids], expert_id, expert_gate, expert_up, expert_down)
        factor = jnp.where(live, flat_weight[picks], jnp.float32(0.0))
        return (total.at[token_ids].add(outputs * factor[:, None]), None)
    ffn_sum, _ = lax.scan(add_expert, jnp.zeros((count, D), jnp.float32), jnp.arange(EXPERTS, dtype=jnp.int32))
    return (middle.astype(jnp.float32) + rms_scale(ffn_sum, post_ffn_gain)).astype(jnp.bfloat16)
```

```python
import jax
import jax.numpy as jnp
from jax import lax
from jax.sharding import PartitionSpec as P

GROUPS = 4
TOP = 2
CHUNKS = 2


EPS = 1e-06


def shifted(block, axis, distance):
    devices = range(lax.axis_size(axis))
    route = [(i - distance, i) for i in devices if i - distance in devices]
    return lax.ppermute(block, axis, route)


def rms_scale(values, gain):
    values = values.astype(jnp.float32)
    inverse = lax.rsqrt(jnp.mean(values * values, axis=-1, keepdims=True) + EPS)
    return values * inverse * gain


def window_sums(extended, lookback, count):
    levels = []
    current = extended
    window_span = 1
    for level_id in range(GROUPS):
        current = current[window_span:] + current[:-window_span]
        window_span = window_span * 2
        first = lookback - window_span + 1
        levels.append(lax.slice_in_dim(current, first, first + count, axis=0))
    return levels


def expert_half(token_rows, gate_full, up_full, down_full):
    flat_rows = token_rows.reshape(-1, token_rows.shape[-1])
    gate_value = jnp.dot(flat_rows, gate_full, preferred_element_type=jnp.float32)
    up_value = jnp.dot(flat_rows, up_full, preferred_element_type=jnp.float32)
    active = (jax.nn.silu(gate_value) * up_value).astype(jnp.bfloat16)
    half = jnp.dot(active, down_full, preferred_element_type=jnp.float32)
    return half.astype(jnp.bfloat16).reshape(token_rows.shape)


def body(
    residual,
    projected,
    group_weight,
    channel_scale,
    out_weight,
    post_mix_gain,
    pre_ffn_gain,
    post_ffn_gain,
    route_ids,
    route_weight,
    expert_gate,
    expert_up,
    expert_down,
):
    lookback = 2**GROUPS
    tokens_here = projected.shape[0]
    width_here = projected.shape[1]
    model_width = out_weight.shape[1]
    tp_count = lax.axis_size("tp")
    tp_index = lax.axis_index("tp")
    groups_here = GROUPS // tp_count
    group_width = width_here // groups_here
    earlier = shifted(projected[tokens_here - lookback :], "sp", 1)
    extended = jnp.concatenate([earlier, projected], 0).astype(jnp.float32)
    levels = window_sums(extended, lookback, tokens_here)
    offset = lax.axis_index("sp") * tokens_here
    position = (offset + lax.iota(jnp.int32, tokens_here) + 1).astype(jnp.float32)[:, None]
    pieces = []
    for local_group in range(groups_here):
        group_id = tp_index * groups_here + local_group
        low = local_group * group_width
        summed = jnp.zeros((tokens_here, group_width), jnp.float32)
        window_span = jnp.float32(1.0)
        for level_id in range(GROUPS):
            summed = jnp.where(
                group_id == level_id, levels[level_id][:, low : low + group_width], summed
            )
            window_span = jnp.where(
                group_id == level_id, jnp.float32(2.0 ** (level_id + 1)), window_span
            )
        own_part = projected[:, low : low + group_width].astype(jnp.float32)
        pieces.append(summed / jnp.minimum(position, window_span) - own_part)
    pooled = jnp.concatenate(pieces, 1).astype(jnp.bfloat16)
    grouped = jnp.einsum(
        "tgc,gce->tge",
        pooled.reshape(tokens_here, groups_here, group_width),
        group_weight,
        preferred_element_type=jnp.float32,
    )
    scaled = (grouped.reshape(tokens_here, width_here) * channel_scale).astype(jnp.bfloat16)
    weight_rows = lax.dynamic_slice_in_dim(out_weight, tp_index * width_here, width_here, 0)
    projection = lax.psum_scatter(
        jnp.dot(scaled, weight_rows, preferred_element_type=jnp.float32),
        "tp",
        scatter_dimension=0,
        tiled=True,
    )
    mixed = projection.astype(jnp.bfloat16)
    middle = (residual.astype(jnp.float32) + rms_scale(mixed, post_mix_gain)).astype(jnp.bfloat16)
    normed = rms_scale(middle, pre_ffn_gain).astype(jnp.bfloat16)
    row_count = normed.shape[0]
    experts_all = lax.axis_size("sp") // 2
    capacity = 2 * TOP * row_count // experts_all
    flat_ids = route_ids.reshape(-1)
    onehot = (flat_ids[:, None] == lax.iota(jnp.int32, experts_all)[None, :]).astype(jnp.int32)
    before = jnp.cumsum(onehot, 0) - onehot
    slot_ids = jnp.sum(before * onehot, 1)
    target = flat_ids * capacity + slot_ids
    source_row = lax.iota(jnp.int32, row_count * TOP) // TOP + 1
    source = jnp.zeros((experts_all * capacity,), jnp.int32).at[target].set(source_row)
    filled = source > 0
    table = jnp.where(
        filled[:, None], normed[jnp.maximum(source - 1, 0)], jnp.zeros((), jnp.bfloat16)
    )
    gate_part = expert_gate[0]
    up_part = expert_up[0]
    down_part = expert_down[0]
    gate_full, up_full = (
        lax.all_gather(gate_part, "tp", axis=1, tiled=True),
        lax.all_gather(up_part, "tp", axis=1, tiled=True),
    )
    down_full = lax.all_gather(down_part, "tp", axis=0, tiled=True)
    sp_count = lax.axis_size("sp")
    same_half = [[2 * e + h for e in range(experts_all)] for h in range(2)]
    swap = [(i, i ^ 1) for i in range(sp_count)]

    def exchange(rows):
        return lax.all_to_all(
            rows,
            "sp",
            split_axis=0,
            concat_axis=0,
            axis_index_groups=same_half,
            tiled=True,
        )

    table = table.reshape(experts_all, capacity, model_width)
    step = capacity // CHUNKS
    returned = []
    for chunk in range(CHUNKS):
        own = exchange(table[:, chunk * step : (chunk + 1) * step])
        other = lax.ppermute(own, "sp", swap)
        own_half = expert_half(own, gate_full, up_full, down_full)
        other_half = expert_half(other, gate_full, up_full, down_full)
        peer_half = lax.ppermute(other_half, "sp", swap)
        summed = own_half.astype(jnp.float32) + peer_half.astype(jnp.float32)
        returned.append(exchange(summed.astype(jnp.bfloat16)))
    results = jnp.concatenate(returned, 1)
    picked = results.reshape(experts_all * capacity, model_width)[target].astype(jnp.float32)
    weighted = picked * route_weight.reshape(-1)[:, None]
    ffn_sum = jnp.sum(weighted.reshape(row_count, TOP, model_width), 1)
    return (middle.astype(jnp.float32) + rms_scale(ffn_sum, post_ffn_gain)).astype(jnp.bfloat16)


def solution(mesh):
    in_specs = (
        P(("sp", "tp"), None),
        P("sp", "tp"),
        P("tp", None, None),
        P("tp"),
        P(),
        P(),
        P(),
        P(),
        P(("sp", "tp"), None),
        P(("sp", "tp"), None),
        P("sp", None, "tp"),
        P("sp", None, "tp"),
        P("sp", "tp", None),
    )
    out_specs = P(("sp", "tp"), None)
    return jax.shard_map(body, mesh=mesh, in_specs=in_specs, out_specs=out_specs, check_vma=False)
```

```python
import jax
import jax.numpy as jnp
from jax import lax
from jax.sharding import PartitionSpec as P

GROUPS = 4
TOP = 2
EDGES = (0, 2, 4)
PARTS = 4


EPS = 1e-06


def shifted(block, axis, distance):
    devices = range(lax.axis_size(axis))
    route = [(i - distance, i) for i in devices if i - distance in devices]
    return lax.ppermute(block, axis, route)


def rms_scale(values, gain):
    values = values.astype(jnp.float32)
    inverse = lax.rsqrt(jnp.mean(values * values, axis=-1, keepdims=True) + EPS)
    return values * inverse * gain


def window_sums(extended, lookback, count):
    levels = []
    current = extended
    window_span = 1
    for level_id in range(GROUPS):
        current = current[window_span:] + current[:-window_span]
        window_span = window_span * 2
        first = lookback - window_span + 1
        levels.append(lax.slice_in_dim(current, first, first + count, axis=0))
    return levels


def expert_half(token_rows, gate_full, up_full, down_full):
    flat_rows = token_rows.reshape(-1, token_rows.shape[-1])
    gate_value = jnp.dot(flat_rows, gate_full, preferred_element_type=jnp.float32)
    up_value = jnp.dot(flat_rows, up_full, preferred_element_type=jnp.float32)
    active = (jax.nn.silu(gate_value) * up_value).astype(jnp.bfloat16)
    half = jnp.dot(active, down_full, preferred_element_type=jnp.float32)
    return half.astype(jnp.bfloat16).reshape(token_rows.shape)


def body(
    residual,
    projected,
    group_weight,
    channel_scale,
    out_weight,
    post_mix_gain,
    pre_ffn_gain,
    post_ffn_gain,
    route_ids,
    route_weight,
    expert_gate,
    expert_up,
    expert_down,
):
    lookback = 2**GROUPS
    tokens_here = projected.shape[0]
    width_here = projected.shape[1]
    model_width = out_weight.shape[1]
    tp_count = lax.axis_size("tp")
    tp_index = lax.axis_index("tp")
    groups_here = GROUPS // tp_count
    group_width = width_here // groups_here
    earlier = shifted(projected[tokens_here - lookback :], "sp", 1)
    extended = jnp.concatenate([earlier, projected], 0).astype(jnp.float32)
    levels = window_sums(extended, lookback, tokens_here)
    offset = lax.axis_index("sp") * tokens_here
    position = (offset + lax.iota(jnp.int32, tokens_here) + 1).astype(jnp.float32)[:, None]
    pieces = []
    for local_group in range(groups_here):
        group_id = tp_index * groups_here + local_group
        low = local_group * group_width
        summed = jnp.zeros((tokens_here, group_width), jnp.float32)
        window_span = jnp.float32(1.0)
        for level_id in range(GROUPS):
            summed = jnp.where(
                group_id == level_id, levels[level_id][:, low : low + group_width], summed
            )
            window_span = jnp.where(
                group_id == level_id, jnp.float32(2.0 ** (level_id + 1)), window_span
            )
        own_part = projected[:, low : low + group_width].astype(jnp.float32)
        pieces.append(summed / jnp.minimum(position, window_span) - own_part)
    pooled = jnp.concatenate(pieces, 1).astype(jnp.bfloat16)
    grouped = jnp.einsum(
        "tgc,gce->tge",
        pooled.reshape(tokens_here, groups_here, group_width),
        group_weight,
        preferred_element_type=jnp.float32,
    )
    scaled = (grouped.reshape(tokens_here, width_here) * channel_scale).astype(jnp.bfloat16)
    weight_rows = lax.dynamic_slice_in_dim(out_weight, tp_index * width_here, width_here, 0)
    rows_here = tokens_here // tp_count

    def project(owner):
        block = lax.dynamic_slice_in_dim(scaled, owner * rows_here, rows_here, 0)
        return jnp.dot(block, weight_rows, preferred_element_type=jnp.float32)

    projection = None
    for distance in range(1, tp_count):
        owner = lax.rem(tp_index + distance, tp_count)
        route = [(i, (i + distance) % tp_count) for i in range(tp_count)]
        arrived = lax.ppermute(project(owner), "tp", route)
        projection = arrived if projection is None else projection + arrived
    projection = project(tp_index) + projection
    mixed = projection.astype(jnp.bfloat16)
    middle = (residual.astype(jnp.float32) + rms_scale(mixed, post_mix_gain)).astype(jnp.bfloat16)
    normed = rms_scale(middle, pre_ffn_gain).astype(jnp.bfloat16)
    row_count = normed.shape[0]
    experts_all = lax.axis_size("sp") // 2
    capacity = 2 * TOP * row_count // experts_all
    flat_ids = route_ids.reshape(-1)
    onehot = (flat_ids[:, None] == lax.iota(jnp.int32, experts_all)[None, :]).astype(jnp.int32)
    before = jnp.cumsum(onehot, 0) - onehot
    slot_ids = jnp.sum(before * onehot, 1)
    target = flat_ids * capacity + slot_ids
    source_row = lax.iota(jnp.int32, row_count * TOP) // TOP + 1
    source = jnp.zeros((experts_all * capacity,), jnp.int32).at[target].set(source_row)
    filled = source > 0
    table = jnp.where(
        filled[:, None], normed[jnp.maximum(source - 1, 0)], jnp.zeros((), jnp.bfloat16)
    )
    gate_part = expert_gate[0]
    up_part = expert_up[0]
    down_part = expert_down[0]
    gate_full, up_full = (
        lax.all_gather(gate_part, "tp", axis=1, tiled=True),
        lax.all_gather(up_part, "tp", axis=1, tiled=True),
    )
    down_full = lax.all_gather(down_part, "tp", axis=0, tiled=True)
    sp_count = lax.axis_size("sp")
    same_half = [[2 * e + h for e in range(experts_all)] for h in range(2)]
    swap = [(i, i ^ 1) for i in range(sp_count)]

    def exchange(rows):
        return lax.all_to_all(
            rows,
            "sp",
            split_axis=0,
            concat_axis=0,
            axis_index_groups=same_half,
            tiled=True,
        )

    table = table.reshape(experts_all, capacity, model_width)
    bounds = [capacity * part // PARTS for part in EDGES]
    returned = []
    owns = [exchange(table[:, low:high]) for low, high in zip(bounds[:-1], bounds[1:])]
    for own in owns:
        other = lax.ppermute(own, "sp", swap)
        own_half = expert_half(own, gate_full, up_full, down_full)
        other_half = expert_half(other, gate_full, up_full, down_full)
        peer_half = lax.ppermute(other_half, "sp", swap)
        summed = own_half.astype(jnp.float32) + peer_half.astype(jnp.float32)
        returned.append(exchange(summed.astype(jnp.bfloat16)))
    results = jnp.concatenate(returned, 1)
    picked = results.reshape(experts_all * capacity, model_width)[target].astype(jnp.float32)
    weighted = picked * route_weight.reshape(-1)[:, None]
    ffn_sum = jnp.sum(weighted.reshape(row_count, TOP, model_width), 1)
    return (middle.astype(jnp.float32) + rms_scale(ffn_sum, post_ffn_gain)).astype(jnp.bfloat16)


def solution(mesh):
    in_specs = (
        P(("sp", "tp"), None),
        P("sp", "tp"),
        P("tp", None, None),
        P("tp"),
        P(),
        P(),
        P(),
        P(),
        P(("sp", "tp"), None),
        P(("sp", "tp"), None),
        P("sp", None, "tp"),
        P("sp", None, "tp"),
        P("sp", "tp", None),
    )
    out_specs = P(("sp", "tp"), None)
    return jax.shard_map(body, mesh=mesh, in_specs=in_specs, out_specs=out_specs, check_vma=False)
```
